32 devices in a mesh: fs: 16 (over z, y, x), tp: 2 (over core).
Axes of the slice: x: 2, y: 2, z: 4, core: 2. Of those that a mesh axis runs over, the one named last changes fastest.
Arguments:
- fwd_input: bfloat16 [2048, 2048], P('fs'), may hold values from -6 to 6
- saved_input: bfloat16 [2048, 2048], P('fs'), may hold values from -6 to 6
- out_cotangent: bfloat16 [2048, 2048], P('fs'), may hold values from -6 to 6
- up_weight: bfloat16 [2048, 4096], P('fs', 'tp'), may hold values from -0.125 to 0.125
- down_weight: bfloat16 [4096, 2048], P('tp', 'fs'), may hold values from -0.09375 to 0.09375
- up_grad_sum: float32 [2048, 4096], P('fs', 'tp'), may hold values from -6 to 6
Outputs:
- layer_out: bfloat16 [2048, 2048], P('fs')
- input_grad: bfloat16 [2048, 2048], P('fs')
- up_grad_out: float32 [2048, 4096], P('fs', 'tp')
The draws below stay inside these ranges and needn't reach their ends.
All inputs are finite; a program needn't handle non-finite values.
Results may differ from the reference program's by a relative error of at most 0.013.
Values may be sent and summed in bfloat16 or wider, within the bound.
A program may use at most 128 MiB of HBM per device.

```python
import jax
import jax.numpy as jnp
from jax import lax

D = 2048
FF = 4096
TOKENS = 2048
N_TP = 2


def spiked(entries, key, source, target, parts, factor):
    owner, partner = [(jnp.arange(entries.shape[axis_at]) // (entries.shape[axis_at] // parts)).reshape([-1 if axis == axis_at else 1 for axis in range(entries.ndim)]) for axis_at in (source, target)]
    chosen = jax.random.permutation(key, parts)[partner]
    strong = (owner == chosen) | (owner == (partner + parts // 2) % parts)
    return jnp.where(strong, factor * entries, entries)


def level_of(own_key, dims, cuts, least, top_value):
    loudness, own = 1.0, jax.random.fold_in(own_key, 6)
    for position, shards_of in cuts:
        steps = jnp.exp(jax.random.uniform(jax.random.fold_in(own, position), (shards_of,), jnp.float32, least / len(cuts), top_value / len(cuts)))
        loudness = loudness * jnp.repeat(steps, dims[position] // shards_of).reshape([-1 if axis == position else 1 for axis in range(len(dims))])
    return loudness


def centred(stream_key, dims, spread, limit, cuts=(), held_as=jnp.bfloat16):
    loudness = level_of(stream_key, dims, cuts, -0.22, 0.18) if cuts else 1.0
    drawn = jax.random.normal(stream_key, dims, jnp.float32) * spread * loudness
    return jnp.minimum(jnp.maximum(drawn, -limit), limit).astype(held_as)


def bell_draw_with(key, shape, scale, most, pieces, heavy, dtype=jnp.bfloat16):
    values = scale * jax.random.normal(key, shape, jnp.float32)
    if pieces:
        values = values * level_of(key, shape, pieces, -0.22, 0.18)
    return jnp.clip(spiked(values, jax.random.fold_in(key, 3), *heavy), -most, most).astype(dtype)


def setup_inputs(seed: int = 0) -> dict:
    splits = jax.random.split(jax.random.key(seed), 7)
    fwd_input = centred(splits[0], (TOKENS, D), 1.0, 6.0, ((0, 16),))
    saved_input = bell_draw_with(splits[1], (TOKENS, D), 1.0, 6.0, ((0, 16),), (0, 1, 16, 2.0))
    out_cotangent = bell_draw_with(splits[2], (TOKENS, D), 1.0, 6.0, ((0, 16),), (0, 1, 16, 2.0))
    up_weight = centred(splits[3], (D, FF), D ** -0.5, 0.125, ((0, 16), (1, 2)))
    down_weight = centred(splits[4], (FF, D), FF ** -0.5, 0.09375, ((0, 2), (1, 16)))
    up_grad_sum = centred(splits[5], (D, FF), 1.0, 6.0, ((0, 16), (1, 2)), jnp.float32)
    return {"fwd_input": fwd_input, "saved_input": saved_input, "out_cotangent": out_cotangent, "up_weight": up_weight, "down_weight": down_weight, "up_grad_sum": up_grad_sum}


def split_sum(left, right):
    block = right.shape[0] // N_TP
    running = jnp.zeros((left.shape[0], right.shape[1]), jnp.float32)
    for index in range(N_TP):
        partial_out = jnp.dot(left[:, index * block:(index + 1) * block], right[index * block:(index + 1) * block], preferred_element_type=jnp.float32)
        rounded = lax.optimization_barrier(partial_out.astype(jnp.bfloat16))
        running = running + rounded.astype(jnp.float32)
    return running.astype(jnp.bfloat16)


def reference(fwd_input, saved_input, out_cotangent, up_weight, down_weight, up_grad_sum):
    pre_fwd = jnp.dot(fwd_input, up_weight, preferred_element_type=jnp.float32)
    positive = jnp.maximum(pre_fwd, 0.0)
    hidden = (positive * positive).astype(jnp.bfloat16)
    layer_out = split_sum(hidden, down_weight)
    pre_bwd = jnp.dot(saved_input, up_weight, preferred_element_type=jnp.float32)
    d_hidden = jnp.dot(out_cotangent, down_weight.T, preferred_element_type=jnp.float32)
    d_pre = (d_hidden * 2.0 * jnp.maximum(pre_bwd, 0.0)).astype(jnp.bfloat16)
    input_grad = split_sum(d_pre, up_weight.T)
    up_grad = jnp.dot(saved_input.T, d_pre, preferred_element_type=jnp.float32)
    up_grad_out = up_grad_sum + up_grad * (float(TOKENS) ** -0.5)
    return layer_out, input_grad, up_grad_out
```

```python
import functools

import jax
import jax.numpy as jnp
from jax import lax
from jax.experimental import pallas as pl
from jax.experimental.pallas import tpu as pltpu
from jax.sharding import PartitionSpec as P

MESH = pl.DeviceIdType.MESH
F32 = jnp.float32
BF16 = jnp.bfloat16


def remote(src, dst, send_sem, recv_sem, fs, tp):
    return pltpu.make_async_remote_copy(
        src_ref=src,
        dst_ref=dst,
        send_sem=send_sem,
        recv_sem=recv_sem,
        device_id=(fs, tp),
        device_id_type=MESH,
    )


def kernel(
    n, T, B, fwd, saved, cot, up, down_t, out, ing, gout,
    X, W, H, O, tp_in, S, pl_in, G, from_left, from_right,
    lsem, wS, wR, zS, zR, aS, aR, bS, bR, tS, tR, pS, pR, fS, fR, gS, gL, gR, hS, hR,
):
    A = n // B
    f, t = lax.axis_index("fs"), lax.axis_index("tp")
    z, p = lax.div(f, B), lax.rem(f, B)
    rows, D = fwd.shape
    C = rows // T
    Rw, F = up.shape
    Fs = F // B
    tokens = B * rows
    peers = [lax.rem(p + i, B) for i in range(1, B)]
    mates = [lax.rem(t + i, T) for i in range(1, T)]
    has_left, has_right = z > 0, z < A - 1

    def chunk(index):
        return pl.ds(pl.multiple_of(index * C, C), C)

    def cols(index):
        return pl.ds(pl.multiple_of(index * Fs, Fs), Fs)

    barrier = pltpu.get_barrier_semaphore()
    for q in peers:
        pl.semaphore_signal(barrier, inc=1, device_id=(z * B + q, t), device_id_type=MESH)
    for m in mates:
        pl.semaphore_signal(barrier, inc=1, device_id=(f, m), device_id_type=MESH)

    @pl.when(has_left)
    def _():
        pl.semaphore_signal(barrier, inc=1, device_id=(f - B, t), device_id_type=MESH)

    @pl.when(has_right)
    def _():
        pl.semaphore_signal(barrier, inc=1, device_id=(f + B, t), device_id_type=MESH)

    ends = lax.div(z + A - 1, A) + lax.div(A - 1 - z + A - 1, A)
    pl.semaphore_wait(barrier, B - 1 + T - 1 + ends)

    weights = (up, down_t)

    def slice_out(pc, i, q):
        return remote(
            weights[pc].at[:, cols(q)], W.at[pc, f], wS.at[pc, i], wR.at[pc, p], z * B + q, t
        )

    def slice_in(pc, q):
        return remote(
            W.at[pc, z * B + q], W.at[pc, z * B + q], wS.at[pc, 0], wR.at[pc, q], z * B + q, t
        )

    def line(pc, k, q, way, src=None):
        at = k * B + q
        block = W.at[pc, at]
        target = f + B if way == 0 else f - B
        return remote(block if src is None else src, block, zS.at[way, pc, at], zR.at[pc, at], target, t)

    own_w = [
        pltpu.make_async_copy(weights[pc].at[:, cols(p)], W.at[pc, f], lsem.at[pc]) for pc in range(2)
    ]
    for pc in range(2):
        own_w[pc].start()
        for i, q in enumerate(peers):
            slice_out(pc, i, q).start()
        src = weights[pc].at[:, cols(p)]

        @pl.when(has_right)
        def _(pc=pc, src=src):
            line(pc, z, p, 0, src).start()

        @pl.when(has_left)
        def _(pc=pc, src=src):
            line(pc, z, p, 1, src).start()

    acts = (fwd, saved, cot)

    def act_out(j, i, q):
        return remote(acts[j].at[chunk(t)], X.at[j, p, chunk(t)], aS.at[j, i], aR.at[j, p], z * B + q, t)

    def act_in(j, q):
        there = X.at[j, q, chunk(t)]
        return remote(there, there, aS.at[j, 0], aR.at[j, q], z * B + q, t)

    own_x = [pltpu.make_async_copy(acts[j], X.at[j, p], lsem.at[2 + j]) for j in range(3)]
    for j in (1, 2, 0):
        own_x[j].start()
        for i, q in enumerate(peers):
            act_out(j, i, q).start()

    def act_share(i, q, o, m):
        there = X.at[:, q, chunk(t)]
        return remote(there, there, bS.at[i, o], bR.at[q, t], f, m)

    def act_shared(i, q, o, m):
        there = X.at[:, q, chunk(m)]
        return remote(there, there, bS.at[i, o], bR.at[q, m], f, m)

    for pc in range(2):
        for q in peers:
            slice_in(pc, q).wait_recv()

            @pl.when(has_right)
            def _(pc=pc, q=q):
                line(pc, z, q, 0).start()

            @pl.when(has_left)
            def _(pc=pc, q=q):
                line(pc, z, q, 1).start()

    order = [p] + peers
    for s in range(1, A):
        for pc in range(2):
            for q in order:

                @pl.when(z >= s)
                def _(pc=pc, q=q, s=s):
                    line(pc, z - s, q, 0).wait_recv()

                    @pl.when(has_right)
                    def _():
                        line(pc, z - s, q, 0).start()

                @pl.when(z + s < A)
                def _(pc=pc, q=q, s=s):
                    line(pc, z + s, q, 1).wait_recv()

                    @pl.when(has_left)
                    def _():
                        line(pc, z + s, q, 1).start()

        if s == max(A - 2, 1):
            for i, q in enumerate(peers):
                for j in range(3):
                    act_in(j, q).wait_recv()
                for o, m in enumerate(mates):
                    act_share(i, q, o, m).start()

    for copy in own_w + own_x:
        copy.wait()
    for i, q in enumerate(peers):
        for o, m in enumerate(mates):
            act_shared(i, q, o, m).wait_recv()

    wide = min(256, Fs)

    def product(j, pc, at):
        return jnp.dot(
            X[j].reshape(tokens, D), W[pc, :, :, at].reshape(D, wide), preferred_element_type=F32
        )

    @pl.loop(0, Fs // wide)
    def _(c):
        at = pl.ds(pl.multiple_of(c * wide, wide), wide)
        pre = product(1, 0, at)
        d_hidden = product(2, 1, at)
        H[1, :, at] = (d_hidden * 2.0 * jnp.maximum(pre, 0.0)).astype(BF16)

    def to_right(d):
        return remote(G.at[d], from_left.at[d], gS.at[d], gL.at[d], f + B, t)

    def to_left(d):
        return remote(G.at[d], from_right.at[d], gS.at[d], gR.at[d], f - B, t)

    planes = []
    for i in range((A + 1) // 2):
        planes += [A - 1 - i] if A - 1 - i == i else [A - 1 - i, i]
    deep = B * Rw
    for d in planes:
        term = lax.dot_general(
            X[1, :, :, d * deep:(d + 1) * deep].reshape(tokens, deep),
            H[1],
            (((0,), (0,)), ((), ())),
            preferred_element_type=F32,
        )
        G[d] = term.astype(BF16).reshape(B, Rw, Fs)
        if d > 0:

            @pl.when(z == 0)
            def _(d=d):
                to_right(d).start()

        if d < A - 1:

            @pl.when(z == A - 1)
            def _(d=d):
                to_left(d).start()

    pack = max(1, 256 // Rw)

    def spread(o, pc):
        @pl.loop(0, n // pack)
        def _(c):
            block = W[pc, pl.ds(c * pack, pack)].reshape(pack * Rw, Fs)
            part = lax.dot_general(H[o], block, (((1,), (1,)), ((), ())), preferred_element_type=F32)
            at = pl.ds(pl.multiple_of(c * (pack * Rw), pack * Rw), pack * Rw)
            O[o, :, :, at] = part.astype(BF16).reshape(B, rows, pack * Rw)

    def tp_out(o, i, m):
        return remote(O.at[o, :, chunk(m)], tp_in.at[o, t], tS.at[o, i], tR.at[o, t], f, m)

    def tp_got(o, i, m):
        return remote(tp_in.at[o, m], tp_in.at[o, m], tS.at[o, i], tR.at[o, m], f, m)

    spread(1, 0)
    for i, m in enumerate(mates):
        tp_out(1, i, m).start()

    @pl.loop(0, Fs // wide)
    def _(c):
        at = pl.ds(pl.multiple_of(c * wide, wide), wide)
        positive = jnp.maximum(product(0, 0, at), 0.0)
        H[0, :, at] = (positive * positive).astype(BF16)

    spread(0, 1)
    for i, m in enumerate(mates):
        tp_out(0, i, m).start()

    def plane_out(o, i, q):
        return remote(S.at[o, q], pl_in.at[o, p], pS.at[o, i], pR.at[o, p], z * B + q, t)

    def plane_got(o, i, q):
        return remote(pl_in.at[o, q], pl_in.at[o, q], pS.at[o, i], pR.at[o, q], z * B + q, t)

    for o in (1, 0):
        for i, m in enumerate(mates):
            tp_got(o, i, m).wait_recv()
        for q in peers + [p]:
            total = O[o, q, chunk(t)].astype(F32)
            for m in mates:
                total = total + tp_in[o, m, q].astype(F32)
            S[o, q] = total.astype(BF16)
        for i, q in enumerate(peers):
            plane_out(o, i, q).start()

    for i in range(A - 1):
        right_d, left_d = A - 1 - i, i

        @pl.when(jnp.logical_and(has_left, z < right_d))
        def _(d=right_d):
            to_right(d).wait_recv()
            G[d] = (G[d].astype(F32) + from_left[d].astype(F32)).astype(BF16)
            to_right(d).start()

        @pl.when(jnp.logical_and(has_right, z > left_d))
        def _(d=left_d):
            remote(from_right.at[d], from_right.at[d], gS.at[d], gR.at[d], f, t).wait_recv()
            G[d] = (G[d].astype(F32) + from_right[d].astype(F32)).astype(BF16)
            to_left(d).start()

    outs = (out, ing)

    def share(o, i, m):
        there = outs[o].at[chunk(t)]
        return remote(there, there, fS.at[o, i], fR.at[o, t], f, m)

    def shared(o, i, m):
        there = outs[o].at[chunk(m)]
        return remote(there, there, fS.at[o, i], fR.at[o, m], f, m)

    for o in (1, 0):
        total = S[o, p].astype(F32)
        for i, q in enumerate(peers):
            plane_got(o, i, q).wait_recv()
            total = total + pl_in[o, q].astype(F32)
        outs[o][chunk(t)] = total.astype(BF16)
        for i, m in enumerate(mates):
            share(o, i, m).start()

    @pl.when(has_left)
    def _():
        remote(from_left.at[z], from_left.at[z], gS.at[z], gL.at[z], f, t).wait_recv()
        G[z] = (G[z].astype(F32) + from_left[z].astype(F32)).astype(BF16)

    @pl.when(has_right)
    def _():
        remote(from_right.at[z], from_right.at[z], gS.at[z], gR.at[z], f, t).wait_recv()
        G[z] = (G[z].astype(F32) + from_right[z].astype(F32)).astype(BF16)

    def grad_out(i, q):
        return remote(G.at[z, q], gout.at[p], hS.at[i], hR.at[p], z * B + q, t)

    for i, q in enumerate(peers):
        grad_out(i, q).start()
    gout[p] = G[z, p]

    for i, q in enumerate(peers):
        remote(gout.at[q], gout.at[q], hS.at[i], hR.at[q], z * B + q, t).wait_recv()
        grad_out(i, q).wait_send()
        for pc in range(2):
            slice_out(pc, i, q).wait_send()
        for j in range(3):
            act_out(j, i, q).wait_send()
        for o, m in enumerate(mates):
            act_share(i, q, o, m).wait_send()
        for o in range(2):
            plane_out(o, i, q).wait_send()
    for i, m in enumerate(mates):
        for o in range(2):
            tp_out(o, i, m).wait_send()
            share(o, i, m).wait_send()
            shared(o, i, m).wait_recv()
    for s in range(A):
        for pc in range(2):
            for q in range(B):

                @pl.when(jnp.logical_and(has_right, z >= s))
                def _(pc=pc, q=q, s=s):
                    line(pc, z - s, q, 0).wait_send()

                @pl.when(jnp.logical_and(has_left, z + s < A))
                def _(pc=pc, q=q, s=s):
                    line(pc, z + s, q, 1).wait_send()

    for d in range(A):

        @pl.when(z < d)
        def _(d=d):
            to_right(d).wait_send()

        @pl.when(z > d)
        def _(d=d):
            to_left(d).wait_send()


def groups(n, width):
    size = 1
    while 4 * size * size <= n and n % (2 * size) == 0 and width // (2 * size) >= 128:
        size *= 2
    return size


def per_device(n, T, fwd_input, saved_input, out_cotangent, up_weight, down_weight, up_grad_sum):
    rows, D = fwd_input.shape
    Rw, F = up_weight.shape
    B = groups(n, F)
    A, Fs, C = n // B, F // B, rows // T
    dma = pltpu.SemaphoreType.DMA
    side, mate = max(B - 1, 1), max(T - 1, 1)
    flops = 12 * B * rows * Fs * D
    vmem = pl.BlockSpec(memory_space=pltpu.VMEM)
    layer_out, input_grad, grad = pl.pallas_call(
        functools.partial(kernel, n, T, B),
        out_shape=(
            jax.ShapeDtypeStruct((rows, D), BF16),
            jax.ShapeDtypeStruct((rows, D), BF16),
            jax.ShapeDtypeStruct((B, Rw, Fs), BF16),
        ),
        in_specs=[vmem] * 5,
        out_specs=(vmem,) * 3,
        scratch_shapes=[
            pltpu.VMEM((3, B, rows, D), BF16),
            pltpu.VMEM((2, n, Rw, Fs), BF16),
            pltpu.VMEM((2, B * rows, Fs), BF16),
            pltpu.VMEM((2, B, rows, D), BF16),
            pltpu.VMEM((2, T, B, C, D), BF16),
            pltpu.VMEM((2, B, C, D), BF16),
            pltpu.VMEM((2, B, C, D), BF16),
            pltpu.VMEM((A, B, Rw, Fs), BF16),
            pltpu.VMEM((A, B, Rw, Fs), BF16),
            pltpu.VMEM((A, B, Rw, Fs), BF16),
            dma((5,)),
            dma((2, side)), dma((2, B)),
            dma((2, 2, n)), dma((2, n)),
            dma((3, side)), dma((3, B)),
            dma((side, mate)), dma((B, T)),
            dma((2, mate)), dma((2, T)),
            dma((2, side)), dma((2, B)),
            dma((2, mate)), dma((2, T)),
            dma((A,)), dma((A,)), dma((A,)),
            dma((side,)), dma((B,)),
        ],
        compiler_params=pltpu.CompilerParams(
            collective_id=0, has_side_effects=True, vmem_limit_bytes=58 * 2**20
        ),
        cost_estimate=pl.CostEstimate(flops=flops, bytes_accessed=2**25, transcendentals=0),
    )(fwd_input, saved_input, out_cotangent, up_weight, down_weight.T)
    grad_part = grad.astype(F32).transpose(1, 0, 2).reshape(Rw, F)
    grad_scale = float(rows * n) ** (-0.5)
    return (layer_out, input_grad, up_grad_sum + grad_part * grad_scale)


def solution(mesh):
    placed = (
        P("fs", None),
        P("fs", None),
        P("fs", None),
        P("fs", "tp"),
        P("tp", "fs"),
        P("fs", "tp"),
    )
    return jax.shard_map(
        functools.partial(per_device, mesh.shape["fs"], mesh.shape["tp"]),
        mesh=mesh,
        in_specs=placed,
        out_specs=(P("fs", None), P("fs", None), P("fs", "tp")),
        check_vma=False,
    )
```

```python
import functools

import jax
import jax.numpy as jnp
from jax import lax
from jax.experimental import pallas as pl
from jax.experimental.pallas import tpu as pltpu
from jax.sharding import PartitionSpec as P

MESH = pl.DeviceIdType.MESH
F32 = jnp.float32
BF16 = jnp.bfloat16
PART = 256


def remote(src, dst, send_sem, recv_sem, fs, tp):
    return pltpu.make_async_remote_copy(
        src_ref=src,
        dst_ref=dst,
        send_sem=send_sem,
        recv_sem=recv_sem,
        device_id=(fs, tp),
        device_id_type=MESH,
    )


def kernel(
    n, T, B, Q, fwd, saved, cot, up, down, out, ing, gout,
    X, W, turned, H, O, tp_in, S, pl_in, G, from_left, from_right,
    lsem, wS, wR, zS, zR, aS, aR, bS, bR, tS, tR, pS, pR, fS, fR, gS, gL, gR, hS, hR,
):
    A = n // B
    f, t = lax.axis_index("fs"), lax.axis_index("tp")
    z, p = lax.div(f, B), lax.rem(f, B)
    far = A - 1 - z
    rows, D = fwd.shape
    C = rows // T
    Rw, F = up.shape
    Fs = F // B
    wide = Fs // Q
    tokens = B * rows
    peers = [lax.rem(p + i, B) for i in range(1, B)]
    mates = [lax.rem(t + i, T) for i in range(1, T)]
    has_left, has_right = z > 0, z < A - 1

    def chunk(index):
        return pl.ds(pl.multiple_of(index * C, C), C)

    def cols(index, c):
        return pl.ds(pl.multiple_of(index * Fs + c * wide, wide), wide)

    barrier = pltpu.get_barrier_semaphore()
    for q in peers:
        pl.semaphore_signal(barrier, inc=1, device_id=(z * B + q, t), device_id_type=MESH)
    for m in mates:
        pl.semaphore_signal(barrier, inc=1, device_id=(f, m), device_id_type=MESH)

    @pl.when(has_left)
    def _():
        pl.semaphore_signal(barrier, inc=1, device_id=(f - B, t), device_id_type=MESH)

    @pl.when(has_right)
    def _():
        pl.semaphore_signal(barrier, inc=1, device_id=(f + B, t), device_id_type=MESH)

    ends = lax.div(z + A - 1, A) + lax.div(far + A - 1, A)
    pl.semaphore_wait(barrier, B - 1 + T - 1 + ends)

    weights = (up, down if down.shape == up.shape else turned)

    def slice_out(c, pc, i, q):
        return remote(
            weights[pc].at[:, cols(q, c)], W.at[c, pc, f], wS.at[c, pc, i], wR.at[c, pc, p], z * B + q, t
        )

    def slice_in(c, pc, q):
        there = W.at[c, pc, z * B + q]
        return remote(there, there, wS.at[c, pc, 0], wR.at[c, pc, q], z * B + q, t)

    def line(c, pc, k, q, way, src=None):
        at = k * B + q
        block = W.at[c, pc, at]
        target = f + B if way == 0 else f - B
        return remote(
            block if src is None else src, block, zS.at[way, c, pc, at], zR.at[c, pc, at], target, t
        )

    def own_out(c, pc, q, way):
        src = weights[pc].at[:, cols(p, c)] if q is p else None
        line(c, pc, z, q, way, src).start()

    def both_ways(c, pc, q):
        @pl.when(has_right)
        def _():
            own_out(c, pc, q, 0)

        @pl.when(has_left)
        def _():
            own_out(c, pc, q, 1)

    own_w = [
        pltpu.make_async_copy(weights[pc].at[:, cols(p, c)], W.at[c, pc, f], lsem.at[3 + 2 * c + pc])
        for c in range(Q) for pc in range(2)
    ]
    for c in range(Q):
        for pc in range(2):
            if (c, pc) == (0, 1) and weights[1] is turned:
                turned[...] = down[...].T
            for i, q in enumerate(peers):
                slice_out(c, pc, i, q).start()
            if c == 0:
                both_ways(c, pc, p)
    for copy in own_w:
        copy.start()

    acts = (fwd, saved, cot)

    def act_out(j, i, q):
        return remote(acts[j].at[chunk(t)], X.at[j, p, chunk(t)], aS.at[j, i], aR.at[j, p], z * B + q, t)

    def act_in(j, q):
        there = X.at[j, q, chunk(t)]
        return remote(there, there, aS.at[j, 0], aR.at[j, q], z * B + q, t)

    own_x = [pltpu.make_async_copy(acts[j], X.at[j, p], lsem.at[j]) for j in range(3)]
    for j in (1, 2, 0):
        own_x[j].start()
        for i, q in enumerate(peers):
            act_out(j, i, q).start()

    def act_share(i, q, o, m):
        there = X.at[:, q, chunk(t)]
        return remote(there, there, bS.at[i, o], bR.at[q, t], f, m)

    def act_shared(i, q, o, m):
        there = X.at[:, q, chunk(m)]
        return remote(there, there, bS.at[i, o], bR.at[q, m], f, m)

    for pc in range(2):
        for q in peers:
            slice_in(0, pc, q).wait_recv()
            both_ways(0, pc, q)

    order = [p] + peers

    def gather_step(c, s):
        for pc in range(2):
            for q in order:

                @pl.when(z >= s)
                def _(pc=pc, q=q):
                    line(c, pc, z - s, q, 0).wait_recv()

                    @pl.when(has_right)
                    def _():
                        line(c, pc, z - s, q, 0).start()

                @pl.when(far >= s)
                def _(pc=pc, q=q):
                    line(c, pc, z + s, q, 1).wait_recv()

                    @pl.when(has_left)
                    def _():
                        line(c, pc, z + s, q, 1).start()

        if c == 0 and s == 1:
            for later in range(1, Q):
                for pc in range(2):
                    for q in peers:
                        slice_in(later, pc, q).wait_recv()
        if c + 1 < Q:
            @pl.when(jnp.logical_and(has_right, z == s if s > 1 else z <= 1))
            def _():
                for pc in range(2):
                    for q in order:
                        own_out(c + 1, pc, q, 0)

            @pl.when(jnp.logical_and(has_left, far == s if s > 1 else far <= 1))
            def _():
                for pc in range(2):
                    for q in order:
                        own_out(c + 1, pc, q, 1)

        if c == 0 and s == max(A - 2, 1):
            for i, q in enumerate(peers):
                for j in range(3):
                    act_in(j, q).wait_recv()
                for o, m in enumerate(mates):
                    act_share(i, q, o, m).start()

    def product(c, j, pc):
        return jnp.dot(
            X[j].reshape(tokens, D), W[c, pc].reshape(D, wide), preferred_element_type=F32
        )

    def to_right(c, d):
        return remote(G.at[c, d], from_left.at[c, d], gS.at[c, d], gL.at[c, d], f + B, t)

    def to_left(c, d):
        return remote(G.at[c, d], from_right.at[c, d], gS.at[c, d], gR.at[c, d], f - B, t)

    def add_left(c, d):
        remote(from_left.at[c, d], from_left.at[c, d], gS.at[c, d], gL.at[c, d], f - B, t).wait_recv()
        G[c, d] = (G[c, d].astype(F32) + from_left[c, d].astype(F32)).astype(BF16)

    def add_right(c, d):
        remote(from_right.at[c, d], from_right.at[c, d], gS.at[c, d], gR.at[c, d], f + B, t).wait_recv()
        G[c, d] = (G[c, d].astype(F32) + from_right[c, d].astype(F32)).astype(BF16)

    def grad_out(c, i, q):
        return remote(G.at[c, z, q], gout.at[:, cols(p, c)], hS.at[c, i], hR.at[c, p], z * B + q, t)

    def sum_step(c, s):
        if s < A - 1:

            @pl.when(jnp.logical_and(has_left, z <= s))
            def _():
                add_left(c, far - s + 2 * z)
                to_right(c, far - s + 2 * z).start()

            @pl.when(jnp.logical_and(has_right, far <= s))
            def _():
                add_right(c, s - far)
                to_left(c, s - far).start()

        else:

            @pl.when(has_left)
            def _():
                add_left(c, z)

            @pl.when(has_right)
            def _():
                add_right(c, z)

            for i, q in enumerate(peers):
                grad_out(c, i, q).start()
            gout[:, cols(p, c)] = G[c, z, p]

    planes = []
    for i in range((A + 1) // 2):
        planes += [A - 1 - i] if A - 1 - i == i else [A - 1 - i, i]
    deep = B * Rw

    def backward(c):
        pre = product(c, 1, 0)
        d_hidden = product(c, 2, 1)
        H[1, c] = (d_hidden * 2.0 * jnp.maximum(pre, 0.0)).astype(BF16)
        for d in planes:
            term = lax.dot_general(
                X[1, :, :, d * deep:(d + 1) * deep].reshape(tokens, deep),
                H[1, c],
                (((0,), (0,)), ((), ())),
                preferred_element_type=F32,
            )
            G[c, d] = term.astype(BF16).reshape(B, Rw, wide)
            if d > 0:

                @pl.when(z == 0)
                def _(d=d):
                    to_right(c, d).start()

            if d < A - 1:

                @pl.when(far == 0)
                def _(d=d):
                    to_left(c, d).start()

    def forward(c):
        positive = jnp.maximum(product(c, 0, 0), 0.0)
        H[0, c] = (positive * positive).astype(BF16)

    for c in range(Q):
        for s in range(1, A):
            gather_step(c, s)
            if c > 0:
                sum_step(c - 1, s)
        if c == 0:
            for copy in own_w + own_x:
                copy.wait()
            for i, q in enumerate(peers):
                for o, m in enumerate(mates):
                    act_shared(i, q, o, m).wait_recv()
        backward(c)
        if c + 1 < Q:
            forward(c)

    pack = max(1, 256 // Rw)

    def spread(o, pc):
        @pl.loop(0, n // pack)
        def _(g):
            part = 0.0
            for c in range(Q):
                block = W[c, pc, pl.ds(g * pack, pack)].reshape(pack * Rw, wide)
                part += lax.dot_general(
                    H[o, c], block, (((1,), (1,)), ((), ())), preferred_element_type=F32
                )
            at = pl.ds(pl.multiple_of(g * (pack * Rw), pack * Rw), pack * Rw)
            O[o, :, :, at] = part.astype(BF16).reshape(B, rows, pack * Rw)

    def tp_out(o, i, m):
        return remote(O.at[o, :, chunk(m)], tp_in.at[o, t], tS.at[o, i], tR.at[o, t], f, m)

    def tp_got(o, i, m):
        return remote(tp_in.at[o, m], tp_in.at[o, m], tS.at[o, i], tR.at[o, m], f, m)

    def plane_out(o, i, q):
        return remote(S.at[o, q], pl_in.at[o, p], pS.at[o, i], pR.at[o, p], z * B + q, t)

    def plane_got(o, i, q):
        return remote(pl_in.at[o, q], pl_in.at[o, q], pS.at[o, i], pR.at[o, q], z * B + q, t)

    def plane_sums(o):
        for i, m in enumerate(mates):
            tp_got(o, i, m).wait_recv()
        for i, q in enumerate(peers + [p]):
            total = O[o, q, chunk(t)].astype(F32)
            for m in mates:
                total = total + tp_in[o, m, q].astype(F32)
            S[o, q] = total.astype(BF16)
            if i < len(peers):
                plane_out(o, i, q).start()

    spread(1, 0)
    for i, m in enumerate(mates):
        tp_out(1, i, m).start()
    forward(Q - 1)
    plane_sums(1)
    spread(0, 1)
    for i, m in enumerate(mates):
        tp_out(0, i, m).start()
    plane_sums(0)
    for s in range(1, A):
        sum_step(Q - 1, s)

    outs = (out, ing)

    def share(o, i, m):
        there = outs[o].at[chunk(t)]
        return remote(there, there, fS.at[o, i], fR.at[o, t], f, m)

    def shared(o, i, m):
        there = outs[o].at[chunk(m)]
        return remote(there, there, fS.at[o, i], fR.at[o, m], f, m)

    for o in (1, 0):
        total = S[o, p].astype(F32)
        for i, q in enumerate(peers):
            plane_got(o, i, q).wait_recv()
            total = total + pl_in[o, q].astype(F32)
        outs[o][chunk(t)] = total.astype(BF16)
        for i, m in enumerate(mates):
            share(o, i, m).start()

    for i, q in enumerate(peers):
        for c in range(Q):
            there = gout.at[:, cols(q, c)]
            remote(there, there, hS.at[c, i], hR.at[c, q], z * B + q, t).wait_recv()
            grad_out(c, i, q).wait_send()
            for pc in range(2):
                slice_out(c, pc, i, q).wait_send()
        for j in range(3):
            act_out(j, i, q).wait_send()
        for o, m in enumerate(mates):
            act_share(i, q, o, m).wait_send()
        for o in range(2):
            plane_out(o, i, q).wait_send()
    for i, m in enumerate(mates):
        for o in range(2):
            tp_out(o, i, m).wait_send()
            share(o, i, m).wait_send()
            shared(o, i, m).wait_recv()
    for s in range(A):

        @pl.when(jnp.logical_and(has_right, z >= s))
        def _(s=s):
            for c in range(Q):
                for pc in range(2):
                    for q in range(B):
                        line(c, pc, z - s, q, 0).wait_send()

        @pl.when(jnp.logical_and(has_left, far >= s))
        def _(s=s):
            for c in range(Q):
                for pc in range(2):
                    for q in range(B):
                        line(c, pc, z + s, q, 1).wait_send()

    for d in range(A):
        for c in range(Q):

            @pl.when(z < d)
            def _(c=c, d=d):
                to_right(c, d).wait_send()

            @pl.when(z > d)
            def _(c=c, d=d):
                to_left(c, d).wait_send()


def groups(n, width):
    size = 1
    while 4 * size * size <= n and n % (2 * size) == 0 and width // (2 * size) >= 128:
        size *= 2
    return size


def per_device(n, T, fwd_input, saved_input, out_cotangent, up_weight, down_weight, up_grad_sum):
    rows, D = fwd_input.shape
    Rw, F = up_weight.shape
    B = groups(n, F)
    A, Fs, C = n // B, F // B, rows // T
    Q = max(1, Fs // PART)
    wide = Fs // Q
    down = down_weight if Rw % 128 == 0 and down_weight.shape != up_weight.shape else down_weight.T
    dma = pltpu.SemaphoreType.DMA
    side, mate = max(B - 1, 1), max(T - 1, 1)
    flops = 12 * B * rows * Fs * D
    vmem = pl.BlockSpec(memory_space=pltpu.VMEM)
    layer_out, input_grad, grad = pl.pallas_call(
        functools.partial(kernel, n, T, B, Q),
        out_shape=(
            jax.ShapeDtypeStruct((rows, D), BF16),
            jax.ShapeDtypeStruct((rows, D), BF16),
            jax.ShapeDtypeStruct((Rw, F), BF16),
        ),
        in_specs=[vmem] * 5,
        out_specs=(vmem,) * 3,
        scratch_shapes=[
            pltpu.VMEM((3, B, rows, D), BF16),
            pltpu.VMEM((Q, 2, n, Rw, wide), BF16),
            pltpu.VMEM((Rw, F), BF16),
            pltpu.VMEM((2, Q, B * rows, wide), BF16),
            pltpu.VMEM((2, B, rows, D), BF16),
            pltpu.VMEM((2, T, B, C, D), BF16),
            pltpu.VMEM((2, B, C, D), BF16),
            pltpu.VMEM((2, B, C, D), BF16),
            pltpu.VMEM((Q, A, B, Rw, wide), BF16),
            pltpu.VMEM((Q, A, B, Rw, wide), BF16),
            pltpu.VMEM((Q, A, B, Rw, wide), BF16),
            dma((3 + 2 * Q,)),
            dma((Q, 2, side)), dma((Q, 2, B)),
            dma((2, Q, 2, n)), dma((Q, 2, n)),
            dma((3, side)), dma((3, B)),
            dma((side, mate)), dma((B, T)),
            dma((2, mate)), dma((2, T)),
            dma((2, side)), dma((2, B)),
            dma((2, mate)), dma((2, T)),
            dma((Q, A)), dma((Q, A)), dma((Q, A)),
            dma((Q, side)), dma((Q, B)),
        ],
        compiler_params=pltpu.CompilerParams(
            collective_id=0, has_side_effects=True, vmem_limit_bytes=58 * 2**20
        ),
        cost_estimate=pl.CostEstimate(flops=flops, bytes_accessed=2**25, transcendentals=0),
    )(fwd_input, saved_input, out_cotangent, up_weight, down)
    grad_part = grad.astype(F32)
    grad_scale = float(rows * n) ** (-0.5)
    return (layer_out, input_grad, up_grad_sum + grad_part * grad_scale)


def solution(mesh):
    placed = (
        P("fs", None),
        P("fs", None),
        P("fs", None),
        P("fs", "tp"),
        P("tp", "fs"),
        P("fs", "tp"),
    )
    return jax.shard_map(
        functools.partial(per_device, mesh.shape["fs"], mesh.shape["tp"]),
        mesh=mesh,
        in_specs=placed,
        out_specs=(P("fs", None), P("fs", None), P("fs", "tp")),
        check_vma=False,
    )
```

```python
import functools

import jax
import jax.numpy as jnp
from jax import lax
from jax.experimental import pallas as pl
from jax.experimental.pallas import tpu as pltpu
from jax.sharding import PartitionSpec as P

MESH = pl.DeviceIdType.MESH
F32 = jnp.float32
BF16 = jnp.bfloat16
PART = 256


def remote(src, dst, send_sem, recv_sem, fs, tp):
    return pltpu.make_async_remote_copy(
        src_ref=src,
        dst_ref=dst,
        send_sem=send_sem,
        recv_sem=recv_sem,
        device_id=(fs, tp),
        device_id_type=MESH,
    )


def kernel(
    n, T, B, Q, fwd, saved, cot, up, down, out, ing, gout,
    X, W, turned, H, pre, O, tp_in, S, pl_in, G, from_left, from_right,
    lsem, wS, wR, zS, zR, aS, aR, bS, bR, tS, tR, pS, pR, fS, fR, gS, gL, gR, hS, hR,
):
    A = n // B
    f, t = lax.axis_index("fs"), lax.axis_index("tp")
    z, p = lax.div(f, B), lax.rem(f, B)
    far = A - 1 - z
    rows, D = fwd.shape
    C = rows // T
    Rw, F = up.shape
    Fs = F // B
    wide = Fs // Q
    tokens = B * rows
    peers = [lax.rem(p + i, B) for i in range(1, B)]
    mates = [lax.rem(t + i, T) for i in range(1, T)]
    has_left, has_right = z > 0, z < A - 1
    stages = [(c, pc) for pc in range(2) for c in range(Q)]
    last = len(stages) - 1

    def chunk(index):
        return pl.ds(pl.multiple_of(index * C, C), C)

    def cols(index, c):
        return pl.ds(pl.multiple_of(index * Fs + c * wide, wide), wide)

    barrier = pltpu.get_barrier_semaphore()
    for q in peers:
        pl.semaphore_signal(barrier, inc=1, device_id=(z * B + q, t), device_id_type=MESH)
    for m in mates:
        pl.semaphore_signal(barrier, inc=1, device_id=(f, m), device_id_type=MESH)

    @pl.when(has_left)
    def _():
        pl.semaphore_signal(barrier, inc=1, device_id=(f - B, t), device_id_type=MESH)

    @pl.when(has_right)
    def _():
        pl.semaphore_signal(barrier, inc=1, device_id=(f + B, t), device_id_type=MESH)

    ends = lax.div(z + A - 1, A) + lax.div(far + A - 1, A)
    pl.semaphore_wait(barrier, B - 1 + T - 1 + ends)

    weights = (up, down if down.shape == up.shape else turned)

    def slice_out(c, pc, i, q):
        return remote(
            weights[pc].at[:, cols(q, c)], W.at[c, pc, f], wS.at[c, pc, i], wR.at[c, pc, p], z * B + q, t
        )

    def slice_in(c, pc, q):
        there = W.at[c, pc, z * B + q]
        return remote(there, there, wS.at[c, pc, 0], wR.at[c, pc, q], z * B + q, t)

    def line(c, pc, k, q, way, src=None):
        at = k * B + q
        block = W.at[c, pc, at]
        target = f + B if way == 0 else f - B
        return remote(
            block if src is None else src, block, zS.at[way, c, pc, at], zR.at[c, pc, at], target, t
        )

    def own_out(c, pc, q, way):
        src = weights[pc].at[:, cols(p, c)] if q is p else None
        line(c, pc, z, q, way, src).start()

    def both_ways(c, pc, q):
        @pl.when(has_right)
        def _():
            own_out(c, pc, q, 0)

        @pl.when(has_left)
        def _():
            own_out(c, pc, q, 1)

    own_w = [
        pltpu.make_async_copy(weights[pc].at[:, cols(p, c)], W.at[c, pc, f], lsem.at[3 + 2 * c + pc])
        for c, pc in stages
    ]
    for c, pc in stages:
        if (c, pc) == (0, 1) and weights[1] is turned:
            turned[...] = down[...].T
        for i, q in enumerate(peers):
            slice_out(c, pc, i, q).start()
        if (c, pc) == stages[0]:
            both_ways(c, pc, p)
    for copy in own_w:
        copy.start()

    acts = (fwd, saved, cot)

    def act_out(j, i, q):
        return remote(acts[j].at[chunk(t)], X.at[j, p, chunk(t)], aS.at[j, i], aR.at[j, p], z * B + q, t)

    def act_in(j, q):
        there = X.at[j, q, chunk(t)]
        return remote(there, there, aS.at[j, 0], aR.at[j, q], z * B + q, t)

    own_x = [pltpu.make_async_copy(acts[j], X.at[j, p], lsem.at[j]) for j in range(3)]
    for j in (1, 2, 0):
        own_x[j].start()
        for i, q in enumerate(peers):
            act_out(j, i, q).start()

    def act_share(i, q, o, m):
        there = X.at[:, q, chunk(t)]
        return remote(there, there, bS.at[i, o], bR.at[q, t], f, m)

    def act_shared(i, q, o, m):
        there = X.at[:, q, chunk(m)]
        return remote(there, there, bS.at[i, o], bR.at[q, m], f, m)

    for q in peers:
        slice_in(0, 0, q).wait_recv()
        both_ways(0, 0, q)

    order = [p] + peers

    def gather_step(stage, s):
        c, pc = stages[stage]
        for q in order:

            @pl.when(z >= s)
            def _(q=q):
                line(c, pc, z - s, q, 0).wait_recv()

                @pl.when(has_right)
                def _():
                    line(c, pc, z - s, q, 0).start()

            @pl.when(far >= s)
            def _(q=q):
                line(c, pc, z + s, q, 1).wait_recv()

                @pl.when(has_left)
                def _():
                    line(c, pc, z + s, q, 1).start()

        if stage == 0 and s == 1:
            for later in stages[1:]:
                for q in peers:
                    slice_in(*later, q).wait_recv()
        if stage < last:
            @pl.when(jnp.logical_and(has_right, z == s if s > 1 else z <= 1))
            def _():
                for q in order:
                    own_out(*stages[stage + 1], q, 0)

            @pl.when(jnp.logical_and(has_left, far == s if s > 1 else far <= 1))
            def _():
                for q in order:
                    own_out(*stages[stage + 1], q, 1)

        if stage == last - 1 and s == 1:
            for i, q in enumerate(peers):
                for j in range(3):
                    act_in(j, q).wait_recv()
                for o, m in enumerate(mates):
                    act_share(i, q, o, m).start()

    def product(c, j, pc):
        return jnp.dot(
            X[j].reshape(tokens, D), W[c, pc].reshape(D, wide), preferred_element_type=F32
        )

    def to_right(c, d):
        return remote(G.at[c, d], from_left.at[c, d], gS.at[c, d], gL.at[c, d], f + B, t)

    def to_left(c, d):
        return remote(G.at[c, d], from_right.at[c, d], gS.at[c, d], gR.at[c, d], f - B, t)

    def add_left(c, d):
        remote(from_left.at[c, d], from_left.at[c, d], gS.at[c, d], gL.at[c, d], f - B, t).wait_recv()
        G[c, d] = (G[c, d].astype(F32) + from_left[c, d].astype(F32)).astype(BF16)

    def add_right(c, d):
        remote(from_right.at[c, d], from_right.at[c, d], gS.at[c, d], gR.at[c, d], f + B, t).wait_recv()
        G[c, d] = (G[c, d].astype(F32) + from_right[c, d].astype(F32)).astype(BF16)

    def grad_out(c, i, q):
        return remote(G.at[c, z, q], gout.at[:, cols(p, c)], hS.at[c, i], hR.at[c, p], z * B + q, t)

    def sum_step(c, s):
        if s < A - 1:

            @pl.when(jnp.logical_and(has_left, z <= s))
            def _():
                add_left(c, far - s + 2 * z)
                to_right(c, far - s + 2 * z).start()

            @pl.when(jnp.logical_and(has_right, far <= s))
            def _():
                add_right(c, s - far)
                to_left(c, s - far).start()

        else:

            @pl.when(has_left)
            def _():
                add_left(c, z)

            @pl.when(has_right)
            def _():
                add_right(c, z)

            for i, q in enumerate(peers):
                grad_out(c, i, q).start()
            gout[:, cols(p, c)] = G[c, z, p]

    planes = []
    for i in range((A + 1) // 2):
        planes += [A - 1 - i] if A - 1 - i == i else [A - 1 - i, i]
    deep = B * Rw

    def backward(c):
        d_hidden = product(c, 2, 1)
        H[1, c] = (d_hidden * 2.0 * jnp.maximum(pre[c], 0.0)).astype(BF16)
        for d in planes:
            term = lax.dot_general(
                X[1, :, :, d * deep:(d + 1) * deep].reshape(tokens, deep),
                H[1, c],
                (((0,), (0,)), ((), ())),
                preferred_element_type=F32,
            )
            G[c, d] = term.astype(BF16).reshape(B, Rw, wide)
            if d > 0:

                @pl.when(z == 0)
                def _(d=d):
                    to_right(c, d).start()

            if d < A - 1:

                @pl.when(far == 0)
                def _(d=d):
                    to_left(c, d).start()

    def forward(c):
        positive = jnp.maximum(product(c, 0, 0), 0.0)
        H[0, c] = (positive * positive).astype(BF16)
        pre[c] = product(c, 1, 0)

    def columns(k):
        return pl.ds(pl.multiple_of(k * deep, deep), deep)

    def tp_out(o, i, m, k):
        return remote(
            O.at[o, :, chunk(m), columns(k)], tp_in.at[o, t, :, :, columns(k)],
            tS.at[o, i, k], tR.at[o, t, k], f, m,
        )

    def tp_got(o, i, m, k):
        there = tp_in.at[o, m, :, :, columns(k)]
        return remote(there, there, tS.at[o, i, k], tR.at[o, m, k], f, m)

    def plane_out(o, i, q, k):
        return remote(
            S.at[o, q, :, columns(k)], pl_in.at[o, p, :, columns(k)],
            pS.at[o, i, k], pR.at[o, p, k], z * B + q, t,
        )

    def plane_got(o, i, q, k):
        there = pl_in.at[o, q, :, columns(k)]
        return remote(there, there, pS.at[o, i, k], pR.at[o, q, k], z * B + q, t)

    def spread(o, pc, k):
        part = 0.0
        for c in range(Q):
            block = W[c, pc, pl.ds(k * B, B)].reshape(deep, wide)
            part += lax.dot_general(
                H[o, c], block, (((1,), (1,)), ((), ())), preferred_element_type=F32
            )
        O[o, :, :, columns(k)] = part.astype(BF16).reshape(B, rows, deep)
        for i, m in enumerate(mates):
            tp_out(o, i, m, k).start()

    def plane_sums(o, k):
        for i, m in enumerate(mates):
            tp_got(o, i, m, k).wait_recv()
        for i, q in enumerate(peers + [p]):
            total = O[o, q, chunk(t), columns(k)].astype(F32)
            for m in mates:
                total = total + tp_in[o, m, q, :, columns(k)].astype(F32)
            S[o, q, :, columns(k)] = total.astype(BF16)
            if i < len(peers):
                plane_out(o, i, q, k).start()

    def out_step(s, work):
        if s == 0:
            work(z)
            return

        @pl.when(z >= s)
        def _():
            work(z - s)

        @pl.when(far >= s)
        def _():
            work(z + s)

    for stage in range(last + 1):
        c = stage - Q
        for s in range(1, A):
            if stage == last:
                out_step(s - 1, lambda k: spread(0, 1, k))
            gather_step(stage, s)
            if c > 0:
                sum_step(c - 1, s)
            if stage == last:
                out_step(s - 1, lambda k: plane_sums(0, k))
        if stage == last - 1:
            for copy in own_w + own_x:
                copy.wait()
            for i, q in enumerate(peers):
                for o, m in enumerate(mates):
                    act_shared(i, q, o, m).wait_recv()
            for part in range(Q):
                forward(part)
        if c >= 0:
            backward(c)

    spread(1, 0, 0)
    for k in range(1, A):
        spread(1, 0, k)
        plane_sums(1, k - 1)
    out_step(A - 1, lambda k: spread(0, 1, k))
    plane_sums(1, A - 1)
    out_step(A - 1, lambda k: plane_sums(0, k))
    for s in range(1, A):
        sum_step(Q - 1, s)

    outs = (out, ing)

    def share(o, i, m):
        there = outs[o].at[chunk(t)]
        return remote(there, there, fS.at[o, i], fR.at[o, t], f, m)

    def shared(o, i, m):
        there = outs[o].at[chunk(m)]
        return remote(there, there, fS.at[o, i], fR.at[o, m], f, m)

    for o in (0, 1):
        total = S[o, p].astype(F32)
        for i, q in enumerate(peers):
            for k in range(A):
                plane_got(o, i, q, k).wait_recv()
            total = total + pl_in[o, q].astype(F32)
        outs[o][chunk(t)] = total.astype(BF16)
        for i, m in enumerate(mates):
            share(o, i, m).start()

    for i, q in enumerate(peers):
        for c in range(Q):
            there = gout.at[:, cols(q, c)]
            remote(there, there, hS.at[c, i], hR.at[c, q], z * B + q, t).wait_recv()
            grad_out(c, i, q).wait_send()
            for pc in range(2):
                slice_out(c, pc, i, q).wait_send()
        for j in range(3):
            act_out(j, i, q).wait_send()
        for o, m in enumerate(mates):
            act_share(i, q, o, m).wait_send()
        for o in range(2):
            for k in range(A):
                plane_out(o, i, q, k).wait_send()
    for i, m in enumerate(mates):
        for o in range(2):
            for k in range(A):
                tp_out(o, i, m, k).wait_send()
            share(o, i, m).wait_send()
            shared(o, i, m).wait_recv()
    for s in range(A):

        @pl.when(jnp.logical_and(has_right, z >= s))
        def _(s=s):
            for c in range(Q):
                for pc in range(2):
                    for q in range(B):
                        line(c, pc, z - s, q, 0).wait_send()

        @pl.when(jnp.logical_and(has_left, far >= s))
        def _(s=s):
            for c in range(Q):
                for pc in range(2):
                    for q in range(B):
                        line(c, pc, z + s, q, 1).wait_send()

    for d in range(A):
        for c in range(Q):

            @pl.when(z < d)
            def _(c=c, d=d):
                to_right(c, d).wait_send()

            @pl.when(z > d)
            def _(c=c, d=d):
                to_left(c, d).wait_send()


def groups(n, width):
    size = 1
    while 4 * size * size <= n and n % (2 * size) == 0 and width // (2 * size) >= 128:
        size *= 2
    return size


def per_device(n, T, fwd_input, saved_input, out_cotangent, up_weight, down_weight, up_grad_sum):
    rows, D = fwd_input.shape
    Rw, F = up_weight.shape
    B = groups(n, F)
    A, Fs, C = n // B, F // B, rows // T
    Q = max(1, Fs // PART)
    wide = Fs // Q
    down = down_weight if Rw % 128 == 0 and down_weight.shape != up_weight.shape else down_weight.T
    dma = pltpu.SemaphoreType.DMA
    side, mate = max(B - 1, 1), max(T - 1, 1)
    flops = 12 * B * rows * Fs * D
    vmem = pl.BlockSpec(memory_space=pltpu.VMEM)
    layer_out, input_grad, grad = pl.pallas_call(
        functools.partial(kernel, n, T, B, Q),
        out_shape=(
            jax.ShapeDtypeStruct((rows, D), BF16),
            jax.ShapeDtypeStruct((rows, D), BF16),
            jax.ShapeDtypeStruct((Rw, F), BF16),
        ),
        in_specs=[vmem] * 5,
        out_specs=(vmem,) * 3,
        scratch_shapes=[
            pltpu.VMEM((3, B, rows, D), BF16),
            pltpu.VMEM((Q, 2, n, Rw, wide), BF16),
            pltpu.VMEM((Rw, F), BF16),
            pltpu.VMEM((2, Q, B * rows, wide), BF16),
            pltpu.VMEM((Q, B * rows, wide), F32),
            pltpu.VMEM((2, B, rows, D), BF16),
            pltpu.VMEM((2, T, B, C, D), BF16),
            pltpu.VMEM((2, B, C, D), BF16),
            pltpu.VMEM((2, B, C, D), BF16),
            pltpu.VMEM((Q, A, B, Rw, wide), BF16),
            pltpu.VMEM((Q, A, B, Rw, wide), BF16),
            pltpu.VMEM((Q, A, B, Rw, wide), BF16),
            dma((3 + 2 * Q,)),
            dma((Q, 2, side)), dma((Q, 2, B)),
            dma((2, Q, 2, n)), dma((Q, 2, n)),
            dma((3, side)), dma((3, B)),
            dma((side, mate)), dma((B, T)),
            dma((2, mate, A)), dma((2, T, A)),
            dma((2, side, A)), dma((2, B, A)),
            dma((2, mate)), dma((2, T)),
            dma((Q, A)), dma((Q, A)), dma((Q, A)),
            dma((Q, side)), dma((Q, B)),
        ],
        compiler_params=pltpu.CompilerParams(
            collective_id=0, has_side_effects=True, vmem_limit_bytes=58 * 2**20
        ),
        cost_estimate=pl.CostEstimate(flops=flops, bytes_accessed=2**25, transcendentals=0),
    )(fwd_input, saved_input, out_cotangent, up_weight, down)
    grad_part = grad.astype(F32)
    grad_scale = float(rows * n) ** (-0.5)
    return (layer_out, input_grad, up_grad_sum + grad_part * grad_scale)


def solution(mesh):
    placed = (
        P("fs", None),
        P("fs", None),
        P("fs", None),
        P("fs", "tp"),
        P("tp", "fs"),
        P("fs", "tp"),
    )
    return jax.shard_map(
        functools.partial(per_device, mesh.shape["fs"], mesh.shape["tp"]),
        mesh=mesh,
        in_specs=placed,
        out_specs=(P("fs", None), P("fs", None), P("fs", "tp")),
        check_vma=False,
    )
```

```python
import functools

import jax
import jax.numpy as jnp
from jax import lax
from jax.experimental import pallas as pl
from jax.experimental.pallas import tpu as pltpu
from jax.sharding import PartitionSpec as P

MESH = pl.DeviceIdType.MESH
F32 = jnp.float32
BF16 = jnp.bfloat16
PART = 256


def remote(src, dst, send_sem, recv_sem, fs, tp):
    return pltpu.make_async_remote_copy(
        src_ref=src,
        dst_ref=dst,
        send_sem=send_sem,
        recv_sem=recv_sem,
        device_id=(fs, tp),
        device_id_type=MESH,
    )


def kernel(
    n, T, B, Q, fwd, saved, cot, up, down, out, ing, gout,
    X, W, turned, H, pre, O, tp_in, S, pl_in, G, from_left, from_right,
    lsem, wS, wR, zS, zR, aS, aR, bS, bR, tS, tR, pS, pR, fS, fR, gS, gL, gR, hS, hR,
):
    A = n // B
    f, t = lax.axis_index("fs"), lax.axis_index("tp")
    z, p = lax.div(f, B), lax.rem(f, B)
    far = A - 1 - z
    rows, D = fwd.shape
    C = rows // T
    Rw, F = up.shape
    Fs = F // B
    wide = Fs // Q
    tokens = B * rows
    peers = [lax.rem(p + i, B) for i in range(1, B)]
    mates = [lax.rem(t + i, T) for i in range(1, T)]
    has_left, has_right = z > 0, z < A - 1
    stages = [(c, pc) for pc in range(2) for c in range(Q)]
    last = len(stages) - 1

    def chunk(index):
        return pl.ds(pl.multiple_of(index * C, C), C)

    def cols(index, c):
        return pl.ds(pl.multiple_of(index * Fs + c * wide, wide), wide)

    barrier = pltpu.get_barrier_semaphore()
    for q in peers:
        pl.semaphore_signal(barrier, inc=1, device_id=(z * B + q, t), device_id_type=MESH)
    for m in mates:
        pl.semaphore_signal(barrier, inc=1, device_id=(f, m), device_id_type=MESH)

    @pl.when(has_left)
    def _():
        pl.semaphore_signal(barrier, inc=1, device_id=(f - B, t), device_id_type=MESH)

    @pl.when(has_right)
    def _():
        pl.semaphore_signal(barrier, inc=1, device_id=(f + B, t), device_id_type=MESH)

    ends = lax.div(z + A - 1, A) + lax.div(far + A - 1, A)
    pl.semaphore_wait(barrier, B - 1 + T - 1 + ends)

    weights = (up, down if down.shape == up.shape else turned)

    def slice_out(c, pc, i, q):
        return remote(
            weights[pc].at[:, cols(q, c)], W.at[c, pc, f], wS.at[c, pc, i], wR.at[c, pc, p], z * B + q, t
        )

    def slice_in(c, pc, q):
        there = W.at[c, pc, z * B + q]
        return remote(there, there, wS.at[c, pc, 0], wR.at[c, pc, q], z * B + q, t)

    def line(c, pc, k, q, way, src=None):
        at = k * B + q
        block = W.at[c, pc, at] if (c, pc) == stages[0] else W.at[c, pc, pl.ds(at, B)]
        target = f + B if way == 0 else f - B
        return remote(
            block if src is None else src, block, zS.at[way, c, pc, at], zR.at[c, pc, at], target, t
        )

    def own_out(c, pc, q, way):
        src = weights[pc].at[:, cols(p, c)] if q is p and (c, pc) == stages[0] else None
        line(c, pc, z, q, way, src).start()

    def both_ways(c, pc, q):
        @pl.when(has_right)
        def _():
            own_out(c, pc, q, 0)

        @pl.when(has_left)
        def _():
            own_out(c, pc, q, 1)

    own_w = [
        pltpu.make_async_copy(weights[pc].at[:, cols(p, c)], W.at[c, pc, f], lsem.at[3 + 2 * c + pc])
        for c, pc in stages
    ]
    for c, pc in stages:
        if (c, pc) == (0, 1) and weights[1] is turned:
            turned[...] = down[...].T
        for i, q in enumerate(peers):
            slice_out(c, pc, i, q).start()
        if (c, pc) == stages[0]:
            both_ways(c, pc, p)
    for copy in own_w:
        copy.start()

    acts = (fwd, saved, cot)

    def act_out(j, i, q):
        return remote(acts[j].at[chunk(t)], X.at[j, p, chunk(t)], aS.at[j, i], aR.at[j, p], z * B + q, t)

    def act_in(j, q):
        there = X.at[j, q, chunk(t)]
        return remote(there, there, aS.at[j, 0], aR.at[j, q], z * B + q, t)

    own_x = [pltpu.make_async_copy(acts[j], X.at[j, p], lsem.at[j]) for j in range(3)]
    for j in (1, 2, 0):
        own_x[j].start()
        for i, q in enumerate(peers):
            act_out(j, i, q).start()

    def act_share(i, q, o, m):
        there = X.at[:, q, chunk(t)]
        return remote(there, there, bS.at[i, o], bR.at[q, t], f, m)

    def act_shared(i, q, o, m):
        there = X.at[:, q, chunk(m)]
        return remote(there, there, bS.at[i, o], bR.at[q, m], f, m)

    for q in peers:
        slice_in(0, 0, q).wait_recv()
        both_ways(0, 0, q)

    order = [p] + peers

    def gather_step(stage, s):
        c, pc = stages[stage]
        for q in order if stage == 0 else (0,):

            @pl.when(z >= s)
            def _(q=q):
                line(c, pc, z - s, q, 0).wait_recv()

                @pl.when(has_right)
                def _():
                    line(c, pc, z - s, q, 0).start()

            @pl.when(far >= s)
            def _(q=q):
                line(c, pc, z + s, q, 1).wait_recv()

                @pl.when(has_left)
                def _():
                    line(c, pc, z + s, q, 1).start()

        if stage == 0 and s == 1:
            for later in stages[1:]:
                for q in peers:
                    slice_in(*later, q).wait_recv()
            for copy in own_w:
                copy.wait()
        if stage < last:
            @pl.when(jnp.logical_and(has_right, z == s if s > 1 else z <= 1))
            def _():
                own_out(*stages[stage + 1], 0, 0)

            @pl.when(jnp.logical_and(has_left, far == s if s > 1 else far <= 1))
            def _():
                own_out(*stages[stage + 1], 0, 1)

        if stage == last - 1 and s == 1:
            for i, q in enumerate(peers):
                for j in range(3):
                    act_in(j, q).wait_recv()
                for o, m in enumerate(mates):
                    act_share(i, q, o, m).start()

    def product(c, j, pc):
        return jnp.dot(
            X[j].reshape(tokens, D), W[c, pc].reshape(D, wide), preferred_element_type=F32
        )

    def to_right(c, d):
        return remote(G.at[c, d], from_left.at[c, d], gS.at[c, d], gL.at[c, d], f + B, t)

    def to_left(c, d):
        return remote(G.at[c, d], from_right.at[c, d], gS.at[c, d], gR.at[c, d], f - B, t)

    def add_left(c, d):
        remote(from_left.at[c, d], from_left.at[c, d], gS.at[c, d], gL.at[c, d], f - B, t).wait_recv()
        G[c, d] = (G[c, d].astype(F32) + from_left[c, d].astype(F32)).astype(BF16)

    def add_right(c, d):
        remote(from_right.at[c, d], from_right.at[c, d], gS.at[c, d], gR.at[c, d], f + B, t).wait_recv()
        G[c, d] = (G[c, d].astype(F32) + from_right[c, d].astype(F32)).astype(BF16)

    def grad_out(c, i, q):
        return remote(G.at[c, z, q], gout.at[:, cols(p, c)], hS.at[c, i], hR.at[c, p], z * B + q, t)

    def sum_step(c, s):
        if s < A - 1:

            @pl.when(jnp.logical_and(has_left, z <= s))
            def _():
                add_left(c, far - s + 2 * z)
                to_right(c, far - s + 2 * z).start()

            @pl.when(jnp.logical_and(has_right, far <= s))
            def _():
                add_right(c, s - far)
                to_left(c, s - far).start()

        else:

            @pl.when(has_left)
            def _():
                add_left(c, z)

            @pl.when(has_right)
            def _():
                add_right(c, z)

            for i, q in enumerate(peers):
                grad_out(c, i, q).start()
            gout[:, cols(p, c)] = G[c, z, p]

    planes = []
    for i in range((A + 1) // 2):
        planes += [A - 1 - i] if A - 1 - i == i else [A - 1 - i, i]
    deep = B * Rw

    def backward(c):
        d_hidden = product(c, 2, 1)
        H[1, c] = (d_hidden * 2.0 * jnp.maximum(pre[c], 0.0)).astype(BF16)
        for d in planes:
            term = lax.dot_general(
                X[1, :, :, d * deep:(d + 1) * deep].reshape(tokens, deep),
                H[1, c],
                (((0,), (0,)), ((), ())),
                preferred_element_type=F32,
            )
            G[c, d] = term.astype(BF16).reshape(B, Rw, wide)
            if d > 0:

                @pl.when(z == 0)
                def _(d=d):
                    to_right(c, d).start()

            if d < A - 1:

                @pl.when(far == 0)
                def _(d=d):
                    to_left(c, d).start()

    def forward(c):
        positive = jnp.maximum(product(c, 0, 0), 0.0)
        H[0, c] = (positive * positive).astype(BF16)
        pre[c] = product(c, 1, 0)

    def columns(k):
        return pl.ds(pl.multiple_of(k * deep, deep), deep)

    def tp_out(o, i, m, k):
        return remote(
            O.at[o, :, chunk(m), columns(k)], tp_in.at[o, t, :, :, columns(k)],
            tS.at[o, i, k], tR.at[o, t, k], f, m,
        )

    def tp_got(o, i, m, k):
        there = tp_in.at[o, m, :, :, columns(k)]
        return remote(there, there, tS.at[o, i, k], tR.at[o, m, k], f, m)

    def plane_out(o, i, q, k):
        return remote(
            S.at[o, q, :, columns(k)], pl_in.at[o, p, :, columns(k)],
            pS.at[o, i, k], pR.at[o, p, k], z * B + q, t,
        )

    def plane_got(o, i, q, k):
        there = pl_in.at[o, q, :, columns(k)]
        return remote(there, there, pS.at[o, i, k], pR.at[o, q, k], z * B + q, t)

    def spread(o, pc, k):
        part = 0.0
        for c in range(Q):
            block = W[c, pc, pl.ds(k * B, B)].reshape(deep, wide)
            part += lax.dot_general(
                H[o, c], block, (((1,), (1,)), ((), ())), preferred_element_type=F32
            )
        O[o, :, :, columns(k)] = part.astype(BF16).reshape(B, rows, deep)
        for i, m in enumerate(mates):
            tp_out(o, i, m, k).start()

    def plane_sums(o, k):
        for i, m in enumerate(mates):
            tp_got(o, i, m, k).wait_recv()
        for i, q in enumerate(peers + [p]):
            total = O[o, q, chunk(t), columns(k)].astype(F32)
            for m in mates:
                total = total + tp_in[o, m, q, :, columns(k)].astype(F32)
            S[o, q, :, columns(k)] = total.astype(BF16)
            if i < len(peers):
                plane_out(o, i, q, k).start()

    def out_step(s, work):
        if s == 0:
            work(z)
            return

        @pl.when(z >= s)
        def _():
            work(z - s)

        @pl.when(far >= s)
        def _():
            work(z + s)

    for stage in range(last + 1):
        c = stage - Q
        for s in range(1, A):
            if stage == last:
                out_step(s - 1, lambda k: spread(0, 1, k))
            gather_step(stage, s)
            if c > 0:
                sum_step(c - 1, s)
            if stage == last:
                out_step(s - 1, lambda k: plane_sums(0, k))
        if stage == last - 1:
            for copy in own_x:
                copy.wait()
            for i, q in enumerate(peers):
                for o, m in enumerate(mates):
                    act_shared(i, q, o, m).wait_recv()
            for part in range(Q):
                forward(part)
        if c >= 0:
            backward(c)

    spread(1, 0, 0)
    for k in range(1, A):
        spread(1, 0, k)
        plane_sums(1, k - 1)
    out_step(A - 1, lambda k: spread(0, 1, k))
    plane_sums(1, A - 1)
    sum_step(Q - 1, 1)
    out_step(A - 1, lambda k: plane_sums(0, k))
    for s in range(2, A):
        sum_step(Q - 1, s)

    outs = (out, ing)

    def share(o, i, m):
        there = outs[o].at[chunk(t)]
        return remote(there, there, fS.at[o, i], fR.at[o, t], f, m)

    def shared(o, i, m):
        there = outs[o].at[chunk(m)]
        return remote(there, there, fS.at[o, i], fR.at[o, m], f, m)

    for o in (0, 1):
        total = S[o, p].astype(F32)
        for i, q in enumerate(peers):
            for k in range(A):
                plane_got(o, i, q, k).wait_recv()
            total = total + pl_in[o, q].astype(F32)
        outs[o][chunk(t)] = total.astype(BF16)
        for i, m in enumerate(mates):
            share(o, i, m).start()

    for i, q in enumerate(peers):
        for c in range(Q):
            there = gout.at[:, cols(q, c)]
            remote(there, there, hS.at[c, i], hR.at[c, q], z * B + q, t).wait_recv()
            grad_out(c, i, q).wait_send()
            for pc in range(2):
                slice_out(c, pc, i, q).wait_send()
        for j in range(3):
            act_out(j, i, q).wait_send()
        for o, m in enumerate(mates):
            act_share(i, q, o, m).wait_send()
        for o in range(2):
            for k in range(A):
                plane_out(o, i, q, k).wait_send()
    for i, m in enumerate(mates):
        for o in range(2):
            for k in range(A):
                tp_out(o, i, m, k).wait_send()
            share(o, i, m).wait_send()
            shared(o, i, m).wait_recv()
    for s in range(A):

        @pl.when(jnp.logical_and(has_right, z >= s))
        def _(s=s):
            for c in range(Q):
                for pc in range(2):
                    for q in range(B if (c, pc) == stages[0] else 1):
                        line(c, pc, z - s, q, 0).wait_send()

        @pl.when(jnp.logical_and(has_left, far >= s))
        def _(s=s):
            for c in range(Q):
                for pc in range(2):
                    for q in range(B if (c, pc) == stages[0] else 1):
                        line(c, pc, z + s, q, 1).wait_send()

    for d in range(A):
        for c in range(Q):

            @pl.when(z < d)
            def _(c=c, d=d):
                to_right(c, d).wait_send()

            @pl.when(z > d)
            def _(c=c, d=d):
                to_left(c, d).wait_send()


def groups(n, width):
    size = 1
    while 4 * size * size <= n and n % (2 * size) == 0 and width // (2 * size) >= 128:
        size *= 2
    return size


def per_device(n, T, fwd_input, saved_input, out_cotangent, up_weight, down_weight, up_grad_sum):
    rows, D = fwd_input.shape
    Rw, F = up_weight.shape
    B = groups(n, F)
    A, Fs, C = n // B, F // B, rows // T
    Q = max(1, Fs // PART)
    wide = Fs // Q
    down = down_weight if Rw % 128 == 0 and down_weight.shape != up_weight.shape else down_weight.T
    dma = pltpu.SemaphoreType.DMA
    side, mate = max(B - 1, 1), max(T - 1, 1)
    flops = 12 * B * rows * Fs * D
    vmem = pl.BlockSpec(memory_space=pltpu.VMEM)
    layer_out, input_grad, grad = pl.pallas_call(
        functools.partial(kernel, n, T, B, Q),
        out_shape=(
            jax.ShapeDtypeStruct((rows, D), BF16),
            jax.ShapeDtypeStruct((rows, D), BF16),
            jax.ShapeDtypeStruct((Rw, F), BF16),
        ),
        in_specs=[vmem] * 5,
        out_specs=(vmem,) * 3,
        scratch_shapes=[
            pltpu.VMEM((3, B, rows, D), BF16),
            pltpu.VMEM((Q, 2, n, Rw, wide), BF16),
            pltpu.VMEM((Rw, F), BF16),
            pltpu.VMEM((2, Q, B * rows, wide), BF16),
            pltpu.VMEM((Q, B * rows, wide), F32),
            pltpu.VMEM((2, B, rows, D), BF16),
            pltpu.VMEM((2, T, B, C, D), BF16),
            pltpu.VMEM((2, B, C, D), BF16),
            pltpu.VMEM((2, B, C, D), BF16),
            pltpu.VMEM((Q, A, B, Rw, wide), BF16),
            pltpu.VMEM((Q, A, B, Rw, wide), BF16),
            pltpu.VMEM((Q, A, B, Rw, wide), BF16),
            dma((3 + 2 * Q,)),
            dma((Q, 2, side)), dma((Q, 2, B)),
            dma((2, Q, 2, n)), dma((Q, 2, n)),
            dma((3, side)), dma((3, B)),
            dma((side, mate)), dma((B, T)),
            dma((2, mate, A)), dma((2, T, A)),
            dma((2, side, A)), dma((2, B, A)),
            dma((2, mate)), dma((2, T)),
            dma((Q, A)), dma((Q, A)), dma((Q, A)),
            dma((Q, side)), dma((Q, B)),
        ],
        compiler_params=pltpu.CompilerParams(
            collective_id=0, has_side_effects=True, vmem_limit_bytes=58 * 2**20
        ),
        cost_estimate=pl.CostEstimate(flops=flops, bytes_accessed=2**25, transcendentals=0),
    )(fwd_input, saved_input, out_cotangent, up_weight, down)
    grad_part = grad.astype(F32)
    grad_scale = float(rows * n) ** (-0.5)
    return (layer_out, input_grad, up_grad_sum + grad_part * grad_scale)


def solution(mesh):
    placed = (
        P("fs", None),
        P("fs", None),
        P("fs", None),
        P("fs", "tp"),
        P("tp", "fs"),
        P("fs", "tp"),
    )
    return jax.shard_map(
        functools.partial(per_device, mesh.shape["fs"], mesh.shape["tp"]),
        mesh=mesh,
        in_specs=placed,
        out_specs=(P("fs", None), P("fs", None), P("fs", "tp")),
        check_vma=False,
    )
```
